128 devices in a mesh: rep: 2 (over z_hi), fs: 32 (over z_lo, y, x), tp: 2 (over core).
Axes of the slice: x: 4, y: 4, z: 4 (z_hi: 2, z_lo: 2; z = z_hi * 2 + z_lo), core: 2. Of those that a mesh axis runs over, the one named last changes fastest.
Arguments:
- tokens: bfloat16 [64, 1024, 2048], P(('rep', 'fs'), 'tp'), may hold values from -6 to 6
- mix_gain: float32 [2048], replicated, may hold values from 0.1 to 1.9
- out_gate_w: float32 [2048, 1024], P('fs', 'tp'), may hold values from -0.125 to 0.125
- in_gate_w: float32 [2048, 1024], P('fs', 'tp'), may hold values from -0.125 to 0.125
- value_w: float32 [2048, 1024], P('fs', 'tp'), may hold values from -0.125 to 0.125
- out_gate_scale: float32 [1024], P(('tp', 'fs')), may hold values from 0.28 to 3.5
- in_gate_scale: float32 [1024], P(('tp', 'fs')), may hold values from 0.5 to 2
- value_scale: float32 [1024], P(('tp', 'fs')), may hold values from 0.5 to 2
- mix_taps: float32 [3, 1024], P(None, 'tp'), may hold values from -3.5 to 3.5
- conv_gain: float32 [1024], P('tp'), may hold values from 0.1 to 1.9
- out_proj_w: float32 [1024, 2048], P('tp', 'fs'), may hold values from -0.1875 to 0.1875
- proj_scale: float32 [2048], P('fs'), may hold values from 0.5 to 2
- ffn_gain: float32 [2048], replicated, may hold values from 0.1 to 1.9
- gate_w: float32 [2048, 2816], P('fs', 'tp'), may hold values from -0.125 to 0.125
- up_w: float32 [2048, 2816], P('fs', 'tp'), may hold values from -0.125 to 0.125
- gate_scale: float32 [2816], P(('tp', 'fs')), may hold values from 0.5 to 2
- up_scale: float32 [2816], P(('tp', 'fs')), may hold values from 0.5 to 2
- gate_taps: float32 [3, 2816], P(None, 'tp'), may hold values from -3.5 to 3.5
- up_taps: float32 [3, 2816], P(None, 'tp'), may hold values from -3.5 to 3.5
- gate_bias: float32 [2816], P('tp'), may hold values from -3 to 3
- up_bias: float32 [2816], P('tp'), may hold values from -3 to 3
- down_w: float32 [2816, 2048], P('tp', 'fs'), may hold values from -0.109375 to 0.109375
- down_scale: float32 [2048], P('fs'), may hold values from 0.5 to 2
Outputs:
- layer_out: bfloat16 [64, 1024, 2048], P(('rep', 'fs'), 'tp')
The draws below stay inside these ranges and needn't reach their ends.
All inputs are finite; a program needn't handle non-finite values.
Results may differ from the reference program's by a relative error of at most 0.02.
Values may be sent and summed in bfloat16 or wider, within the bound.
A program may use at most 128 MiB of HBM per device.

```python
import math
import jax
import jax.numpy as jnp
from jax import lax

D = 2048
CONV = 1024
FF = 2816
KW = 3
SEQ = 1024
SEQS = 64


def draw_out_gate_scale(key, part):
    ramp = jnp.exp(jnp.linspace(math.log(0.4), math.log(2.5), CONV)).astype(jnp.float32)
    noise = jax.random.uniform(key, (CONV,), jnp.float32, 0.7, 1.4)
    return ramp * noise


def block_scale(rng, dims, pieces, low, top_value):
    loudness, own = 1.0, jax.random.fold_in(rng, 6)
    for dim, blocks in pieces:
        steps = jnp.exp(jax.random.uniform(jax.random.fold_in(own, dim), (blocks,), jnp.float32, low / len(pieces), top_value / len(pieces)))
        loudness = loudness * jnp.repeat(steps, dims[dim] // blocks).reshape([-1 if axis == dim else 1 for axis in range(len(dims))])
    return loudness


def bell_draw(key, extent, width, limit, cuts=(), held_as=jnp.bfloat16):
    result = jax.random.normal(key, extent, jnp.float32) * width
    if len(cuts) > 0:
        result = block_scale(key, extent, cuts, -0.22, 0.18) * result
    return jnp.clip(result, min=-limit, max=limit).astype(held_as)


def setup_inputs(seed: int = 0) -> dict:
    streams_of = jax.random.split(jax.random.key(seed), 24)
    tokens = bell_draw(streams_of[0], (SEQS, SEQ, D), 1.0, 6.0, ((0, 64), (1, 2)))
    mix_gain = jnp.clip(1.0 + 0.18 * jax.random.normal(streams_of[1], (D,), jnp.float32), 0.1, 1.9)
    out_gate_w = bell_draw(streams_of[2], (D, CONV), D ** -0.5, 0.125, ((0, 32), (1, 2)), jnp.float32)
    in_gate_w = bell_draw(streams_of[3], (D, CONV), D ** -0.5, 0.125, ((0, 32), (1, 2)), jnp.float32)
    value_w = bell_draw(streams_of[4], (D, CONV), D ** -0.5, 0.125, ((0, 32), (1, 2)), jnp.float32)
    out_gate_scale = draw_out_gate_scale(jax.random.fold_in(streams_of[23], 71), 0)
    in_gate_scale = jnp.clip(jnp.exp(math.log(2.0) - 1.3862944 * jax.random.uniform(streams_of[6], (CONV,), jnp.float32) ** block_scale(streams_of[6], (CONV,), ((0, 64),), -0.2, 0.2)), 0.5, 2.0)
    value_scale = jnp.clip(jnp.exp(math.log(2.0) - 1.3862944 * jax.random.uniform(streams_of[7], (CONV,), jnp.float32) ** block_scale(streams_of[7], (CONV,), ((0, 64),), -0.2, 0.2)), 0.5, 2.0)
    mix_taps = bell_draw(streams_of[8], (KW, CONV), KW ** -0.5, 3.5, ((1, 2),), jnp.float32)
    conv_gain = jnp.clip(1.0 + 0.18 * jax.random.normal(streams_of[9], (CONV,), jnp.float32), 0.1, 1.9)
    out_proj_w = bell_draw(streams_of[10], (CONV, D), CONV ** -0.5, 0.1875, ((0, 2), (1, 32)), jnp.float32)
    proj_scale = jnp.clip(jnp.exp(math.log(2.0) - 1.3862944 * jax.random.uniform(streams_of[11], (D,), jnp.float32) ** block_scale(streams_of[11], (D,), ((0, 32),), -0.2, 0.2)), 0.5, 2.0)
    ffn_gain = jnp.clip(1.0 + 0.18 * jax.random.normal(streams_of[12], (D,), jnp.float32), 0.1, 1.9)
    gate_w = bell_draw(streams_of[13], (D, FF), D ** -0.5, 0.125, ((0, 32), (1, 2)), jnp.float32)
    up_w = bell_draw(streams_of[14], (D, FF), D ** -0.5, 0.125, ((0, 32), (1, 2)), jnp.float32)
    gate_scale = jnp.clip(jnp.exp(math.log(2.0) - 1.3862944 * jax.random.uniform(streams_of[15], (FF,), jnp.float32) ** block_scale(streams_of[15], (FF,), ((0, 64),), -0.2, 0.2)), 0.5, 2.0)
    up_scale = jnp.clip(jnp.exp(math.log(2.0) - 1.3862944 * jax.random.uniform(streams_of[16], (FF,), jnp.float32) ** block_scale(streams_of[16], (FF,), ((0, 64),), -0.2, 0.2)), 0.5, 2.0)
    gate_taps = bell_draw(streams_of[17], (KW, FF), KW ** -0.5, 3.5, ((1, 2),), jnp.float32)
    up_taps = bell_draw(streams_of[18], (KW, FF), KW ** -0.5, 3.5, ((1, 2),), jnp.float32)
    gate_bias = bell_draw(streams_of[19], (FF,), 0.5, 3.0, ((0, 2),), jnp.float32)
    up_bias = bell_draw(streams_of[20], (FF,), 0.5, 3.0, ((0, 2),), jnp.float32)
    down_w = bell_draw(streams_of[21], (FF, D), FF ** -0.5, 0.109375, ((0, 2), (1, 32)), jnp.float32)
    down_scale = jnp.clip(jnp.exp(math.log(2.0) - 1.3862944 * jax.random.uniform(streams_of[22], (D,), jnp.float32) ** block_scale(streams_of[22], (D,), ((0, 32),), -0.2, 0.2)), 0.5, 2.0)
    return {"tokens": tokens, "mix_gain": mix_gain, "out_gate_w": out_gate_w, "in_gate_w": in_gate_w, "value_w": value_w, "out_gate_scale": out_gate_scale, "in_gate_scale": in_gate_scale, "value_scale": value_scale, "mix_taps": mix_taps, "conv_gain": conv_gain, "out_proj_w": out_proj_w, "proj_scale": proj_scale, "ffn_gain": ffn_gain, "gate_w": gate_w, "up_w": up_w, "gate_scale": gate_scale, "up_scale": up_scale, "gate_taps": gate_taps, "up_taps": up_taps, "gate_bias": gate_bias, "up_bias": up_bias, "down_w": down_w, "down_scale": down_scale}


epsilon = 1e-06

def norm_rows(values, gain):
    return values * lax.rsqrt(lax.optimization_barrier(jnp.mean(values * values, axis=-1, keepdims=True)) + epsilon) * gain

def causal_taps(values, taps):
    kernel = taps.shape[0]
    length = values.shape[0]
    padded = jnp.pad(values, ((kernel - 1, 0), (0, 0)))
    total = jnp.zeros(values.shape, jnp.float32)
    for offset in range(kernel):
        total = total + taps[offset] * padded[offset:offset + length]
    return total

def reference(tokens, mix_gain, out_gate_w, in_gate_w, value_w, out_gate_scale, in_gate_scale, value_scale, mix_taps, conv_gain, out_proj_w, proj_scale, ffn_gain, gate_w, up_w, gate_scale, up_scale, gate_taps, up_taps, gate_bias, up_bias, down_w, down_scale):

    def project(left, weight, scale):
        return jnp.dot(left, weight.astype(jnp.bfloat16), preferred_element_type=jnp.float32) * scale

    def layer_one(sequence):
        resid = sequence.astype(jnp.float32)
        normed_in = norm_rows(resid, mix_gain).astype(jnp.bfloat16)
        out_gate = project(normed_in, out_gate_w, out_gate_scale).astype(jnp.bfloat16)
        in_gate = project(normed_in, in_gate_w, in_gate_scale).astype(jnp.bfloat16)
        value_in = project(normed_in, value_w, value_scale).astype(jnp.bfloat16)
        mixed_in = in_gate.astype(jnp.float32) * value_in.astype(jnp.float32)
        conv_out = (out_gate.astype(jnp.float32) * causal_taps(mixed_in, mix_taps)).astype(jnp.bfloat16)
        mixed = norm_rows(conv_out.astype(jnp.float32), conv_gain).astype(jnp.bfloat16)
        first = (resid + project(mixed, out_proj_w, proj_scale)).astype(jnp.bfloat16)
        resid_two = first.astype(jnp.float32)
        normed_ffn = norm_rows(resid_two, ffn_gain).astype(jnp.bfloat16)
        gate_pre = project(normed_ffn, gate_w, gate_scale).astype(jnp.bfloat16)
        up_pre = project(normed_ffn, up_w, up_scale).astype(jnp.bfloat16)
        gate_act = causal_taps(gate_pre.astype(jnp.float32), gate_taps) + gate_bias
        up_act = causal_taps(up_pre.astype(jnp.float32), up_taps) + up_bias
        hidden = (jax.nn.silu(gate_act) * up_act).astype(jnp.bfloat16)
        return (resid_two + project(hidden, down_w, down_scale)).astype(jnp.bfloat16)
    return lax.map(layer_one, tokens)
```

```python
import jax
import jax.numpy as jnp
from jax import lax
from jax.experimental import pallas as pl
from jax.experimental.pallas import tpu as pltpu
from jax.sharding import PartitionSpec as P

EPS = 1e-06
MESH = pl.DeviceIdType.MESH
BF, F32 = jnp.bfloat16, jnp.float32
RATE = 46.65e3
TM = 256

PARTS = (
    ("s", 0, "xyz"),
    ("m", 3, "xyz"),
    ("m", 3, "zxy"),
    ("m", 3, "yxz"),
    ("m", 3, "zyx"),
    ("o", 4, "xyz"),
    ("g", 6, "yxz"),
    ("g", 6, "zxy"),
    ("g", 6, "zyx"),
    ("g", 4, "xyz"),
    ("d", 4, "zxy"),
    ("d", 4, "yxz"),
    ("d", 3, "zyx"),
)


class Copy:
    def __init__(self, part, stage, axis, sign, spec, rows, deps, nbytes):
        self.part, self.stage, self.axis, self.sign = part, stage, axis, sign
        self.spec, self.rows, self.deps, self.nbytes = spec, rows, deps, nbytes
        self.key = (part, stage, 0 if sign > 0 else 1)


def copies_of(part, kind, blocks, order):
    have = dict(x="own", y="own", z="own")
    size = dict(x=4, y=4, z=2)
    row = 512 if kind == "s" else blocks * 256
    whole, halves = ((0, 8), ((0, 8), None)) if kind == "s" else ((0, 64), ((0, 32), (32, 32)))
    made, stage, before = [], 0, []

    def add(stage, axis, sign, spec, rows, deps):
        count = 1
        for a in "xyz":
            count *= size[a] if spec[a] == "all" else 1
        made.append(Copy(part, stage, axis, sign, dict(spec), rows, list(deps), count * rows[1] * row))
        return made[-1].key

    for axis in order:
        done = []
        if axis == "z":
            for sign, rows in zip((1, -1), halves):
                if rows:
                    done.append(add(stage, axis, sign, have, rows, before))
            stage += 1
        else:
            firsts = [add(stage, axis, sign, have, whole, before) for sign in (1, -1)]
            done += firsts
            for sign, first, rows in zip((1, -1), firsts, halves):
                if rows:
                    done.append(add(stage + 1, axis, sign, {**have, axis: -sign}, rows, before + [first]))
            stage += 2
        before = before + done
        have[axis] = "all"
    return made, before


def plan(segments, backlog=4.0, latency=2.4, issue=0.06, start=2.0):
    todo, ends = [], []
    for p, (kind, blocks, order) in enumerate(PARTS):
        made, end = copies_of(p, kind, blocks, order)
        todo += made
        ends.append(end)
    arrive, link = {}, {(a, s): 0.0 for a in "xyz" for s in (1, -1)}
    out, now, seg = [], start, 0
    while todo or seg < len(segments):
        moved = True
        while moved:
            moved = False
            for op in todo:
                if all(arrive.get(d, 1e9) <= now for d in op.deps) and link[op.axis, op.sign] - now < backlog:
                    link[op.axis, op.sign] = max(now, link[op.axis, op.sign]) + op.nbytes / RATE
                    arrive[op.key] = link[op.axis, op.sign] + latency
                    out.append(("send", op, now))
                    now += issue
                    todo.remove(op)
                    moved = True
                    break
        if seg < len(segments):
            name, us, needs = segments[seg]
            if all(arrive.get(k, 1e9) <= now for p in needs for k in ends[p]):
                out.append(("run", segments[seg], now))
                now += us
                seg += 1
                continue
        later = [v for v in arrive.values() if v > now]
        later += [v - backlog + 1e-6 for v in link.values() if v - backlog + 1e-6 > now]
        if not later:
            break
        now = min(later)
    return out, ends


def parts_of(kind):
    return [p for p, part in enumerate(PARTS) if part[0] == kind]


def segments_of():
    out = [("norm", 4.0, [])]
    for c, p in enumerate(parts_of("m")):
        out.append((("m", c, p), 2.4, [p] + parts_of("s")))
    out += [(("o", h), 1.5, parts_of("o")) for h in range(2)]
    out += [(("f", i), 1.5, []) for i in range(4)]
    j = 0
    for p in parts_of("g"):
        for b in range(PARTS[p][1] // 2):
            out.append((("g", j, p, b), 2.0, [p]))
            j += 1
    d = parts_of("d")
    k = 0
    for n, p in enumerate(d[:-1]):
        out += [(("d", p, k, n == 0, h), 1.4, [p]) for h in range(2)]
        k += PARTS[p][1] * 128
    out += [(("e", d[-1], k), 4.0, d[-1:])]
    return out


def dot_nt(a, b):
    return lax.dot_general(a, b, (((1,), (1,)), ((), ())), preferred_element_type=F32)


def shifted_sum(prev, cur, taps):
    both = jnp.concatenate([prev, cur], axis=0)
    one = pltpu.roll(both, 1, 0)[8:]
    two = pltpu.roll(both, 2, 0)[8:]
    return taps[2:3] * cur + taps[1:2] * one + taps[0:1] * two


def kernel(*refs):
    n = len(PARTS)
    (tok, own, sown, mixg, mtaps, cgain, fgain, gtaps, utaps, gbias, ubias, out) = refs[:12]
    bufs = refs[12 : 12 + n]
    (tt, xx, cc, ss, ssr, ps, pr, hh, yy, dr, sc, ssem, rsem, lsem, tsem, trsem) = refs[12 + n :]
    rep, fs, tp = lax.axis_index("rep"), lax.axis_index("fs"), lax.axis_index("tp")
    z, y, x = fs // 16, lax.rem(fs // 4, 4), lax.rem(fs, 4)
    pos = dict(x=x, y=y, z=z)
    mate = (rep, fs, 1 - tp)

    def beside(axis, sign):
        if axis == "x":
            return (rep, z * 16 + y * 4 + lax.rem(x + sign + 4, 4), tp)
        if axis == "y":
            return (rep, z * 16 + lax.rem(y + sign + 4, 4) * 4 + x, tp)
        far = lax.rem(rep * 2 + z + sign + 4, 4)
        return (far // 2, lax.rem(far, 2) * 16 + y * 4 + x, tp)

    local, at = [], 0
    for p, (kind, blocks, _) in enumerate(PARTS):
        src = sown if kind == "s" else own.at[:, pl.ds(at, blocks * 128)]
        local.append(pltpu.make_async_copy(src, bufs[p].at[z, y, x], lsem.at[p]))
        at += blocks * 128
    mine = pl.multiple_of(tp * 512, 512)
    other = pl.multiple_of((1 - tp) * 512, 512)
    local.append(pltpu.make_async_copy(tok.at[0], tt.at[pl.ds(mine, 512)], lsem.at[n]))
    for c in local:
        c.start()

    barrier = pltpu.get_barrier_semaphore()
    for axis in "xyz":
        for sign in (1, -1):
            pl.semaphore_signal(barrier, inc=1, device_id=beside(axis, sign), device_id_type=MESH)
    pl.semaphore_signal(barrier, inc=1, device_id=mate, device_id_type=MESH)
    pl.semaphore_wait(barrier, 7)

    def to_mate(src, dst, k):
        return pltpu.make_async_remote_copy(
            src_ref=src, dst_ref=dst, send_sem=tsem.at[k], recv_sem=trsem.at[k], device_id=mate, device_id_type=MESH
        )

    tokens_over = to_mate(tok.at[0], tt.at[pl.ds(mine, 512)], 0)
    tokens_over.start()
    for c in local:
        c.wait()

    def where(spec, axis):
        v = spec[axis]
        if v == "all":
            return pl.ds(0, 2 if axis == "z" else 4)
        if v == "own":
            return pl.ds(pos[axis], 1)
        return pl.ds(lax.rem(pos[axis] + v + 4, 4), 1)

    def rows_of(i, size=TM):
        return pl.ds(pl.multiple_of(i * size, size), size)

    def whole(p, cols):
        return bufs[p][:, :, :, :, cols].reshape(2048, -1)

    def run_norm():
        tokens_over.wait()

        @pl.loop(0, 1024 // 64)
        def _(i):
            r = rows_of(i, 64)
            v = tt[r, :].astype(F32)
            v = v * lax.rsqrt(jnp.mean(v * v, axis=1, keepdims=True) + EPS) * mixg[...]
            xx[r, :] = v.astype(BF)

    def run_scales(p):
        lane = lax.broadcasted_iota(jnp.int32, (1, 128), 1)
        for k in range(3):
            for b in range(4):
                total = None
                for d in range(8 * b, 8 * b + 8):
                    v = bufs[p][d // 16, d // 4 % 4, d % 4, k : k + 1, :]
                    total = v if total is None else total + v
                sc[k : k + 1, b * 128 : b * 128 + 128] = total
        for k in range(3, 5):
            for b in range(11):
                total = jnp.zeros((1, 128), F32)
                for d in range(32):
                    low, high = max(44 * d - 128 * b, 0), min(44 * d + 44 - 128 * b, 128)
                    if low < high:
                        v = bufs[p][d // 16, d // 4 % 4, d % 4, k : k + 1, :]
                        total = jnp.where((lane >= low) & (lane < high), v, total)
                sc[k : k + 1, b * 128 : b * 128 + 128] = total

    def run_m(c, p):
        cols = slice(c * 128, c * 128 + 128)
        taps, gain = mtaps[:, cols], cgain[:, cols]
        s_out, s_in, s_val = (sc[k : k + 1, cols] for k in range(3))
        s_both = s_in * s_val

        def tile(i, prev):
            r = rows_of(i)
            acc = jnp.dot(xx[r, :], whole(p, slice(None)), preferred_element_type=F32)
            cur = acc[:, 128:256] * acc[:, 256:384] * s_both
            conv = acc[:, 0:128] * s_out * shifted_sum(prev, cur, taps)
            if c == 0:
                ss[r, :] = conv * conv
            else:
                ss[r, :] += conv * conv
            cc[r, cols] = (conv * gain).astype(BF)
            return cur[TM - 8 :]

        lax.fori_loop(0, 1024 // TM, tile, jnp.zeros((8, 128), F32))

    def p_over(i):
        return to_mate(ps.at[rows_of(i)], pr.at[rows_of(i)], 2 + i)

    squares_over = to_mate(ss, ssr, 1)

    def run_o(h):
        (p,) = parts_of("o")

        @pl.loop(2 * h, 2 * h + 2)
        def _(i):
            r = rows_of(i)

            @pl.loop(0, 4)
            def _(q):
                w = bufs[p][q // 2, pl.ds(lax.rem(q, 2) * 2, 2)].reshape(512, 512)
                ps[r, pl.ds(pl.multiple_of(q * 512, 512), 512)] = dot_nt(cc[r, :], w).astype(BF)

        if h == 0:
            squares_over.start()
        else:
            for i in range(4):
                p_over(i).start()

    def run_f(i):
        if i == 0:
            squares_over.wait()
        p_over(i).wait()

        @pl.loop(i * (TM // 64), (i + 1) * (TM // 64))
        def _(k):
            r = rows_of(k, 64)
            row = lax.rsqrt(jnp.sum(ss[r, :] + ssr[r, :], axis=1, keepdims=True) * (1.0 / 1024) + EPS)
            v = tt[r, :].astype(F32) + row * (ps[r, :].astype(F32) + pr[r, :].astype(F32))
            b = v.astype(BF)
            tt[r, :] = b
            v = b.astype(F32)
            v = v * lax.rsqrt(jnp.mean(v * v, axis=1, keepdims=True) + EPS) * fgain[...]
            xx[r, :] = v.astype(BF)

    def run_g(j, p, b):
        cols = slice(j * 128, j * 128 + 128)
        tg, tu, bg, bu = gtaps[:, cols], utaps[:, cols], gbias[:, cols], ubias[:, cols]
        sg, su = sc[3:4, cols], sc[4:5, cols]

        def tile(i, prev):
            r = rows_of(i)
            acc = jnp.dot(xx[r, :], whole(p, slice(b * 256, b * 256 + 256)), preferred_element_type=F32)
            g, u = acc[:, :128] * sg, acc[:, 128:] * su
            ga = shifted_sum(prev[0], g, tg) + bg
            ua = shifted_sum(prev[1], u, tu) + bu
            hh[r, cols] = (ga / (1.0 + jnp.exp(-ga)) * ua).astype(BF)
            return g[TM - 8 :], u[TM - 8 :]

        zero = jnp.zeros((8, 128), F32)
        lax.fori_loop(0, 1024 // TM, tile, (zero, zero))

    def d_tile(r, p, k, q):
        w = bufs[p][q // 2, pl.ds(lax.rem(q, 2) * 2, 2)].reshape(512, -1)
        return dot_nt(hh[r, pl.ds(k, w.shape[1])], w)

    def run_d(p, k, first, h):
        @pl.loop(2 * h, 2 * h + 2)
        def _(i):
            r = rows_of(i)

            @pl.loop(0, 4)
            def _(q):
                c = pl.ds(pl.multiple_of(q * 512, 512), 512)
                if first:
                    yy[r, c] = d_tile(r, p, k, q)
                else:
                    yy[r, c] += d_tile(r, p, k, q)

    def d_over(i):
        return to_mate(ps.at[rows_of(i)], dr.at[rows_of(i)], 6 + i)

    def run_e(p, k):
        for i in range(2):
            r = pl.ds(pl.multiple_of(other + i * TM, TM), TM)

            @pl.loop(0, 4)
            def _(q):
                c = pl.ds(pl.multiple_of(q * 512, 512), 512)
                ps[pl.ds(i * TM, TM), c] = (yy[r, c] + d_tile(r, p, k, q)).astype(BF)

            d_over(i).start()
        for i in range(2):
            r = pl.ds(pl.multiple_of(mine + i * TM, TM), TM)

            @pl.loop(0, 4)
            def _(q):
                c = pl.ds(pl.multiple_of(q * 512, 512), 512)
                yy[r, c] += d_tile(r, p, k, q)

        written = []
        for i in range(2):
            d_over(i).wait()

            @pl.loop(0, TM // 64)
            def _(q):
                r = pl.ds(pl.multiple_of(mine + i * TM + q * 64, 64), 64)
                o = pl.ds(pl.multiple_of(i * TM + q * 64, 64), 64)
                xx[o, :] = (tt[r, :].astype(F32) + yy[r, :] + dr[o, :].astype(F32)).astype(BF)

            w = pltpu.make_async_copy(xx.at[pl.ds(i * TM, TM)], out.at[0, pl.ds(i * TM, TM)], lsem.at[i])
            w.start()
            written.append(w)
        for w in written:
            w.wait()

    steps, ends = plan(segments_of())
    started, got = {}, set()

    def arrived(keys):
        for key in keys:
            if key not in got:
                got.add(key)
                started[key].wait_recv()

    scaled = False
    for what, it, _ in steps:
        if what == "send":
            arrived(it.deps)
            ref = bufs[it.part].at[where(it.spec, "z"), where(it.spec, "y"), where(it.spec, "x"), pl.ds(*it.rows)]
            c = pltpu.make_async_remote_copy(
                src_ref=ref,
                dst_ref=ref,
                send_sem=ssem.at[it.key],
                recv_sem=rsem.at[it.key],
                device_id=beside(it.axis, it.sign),
                device_id_type=MESH,
            )
            c.start()
            started[it.key] = c
            continue
        name, _, needs = it
        for p in needs:
            arrived(ends[p])
        if name == "norm":
            run_norm()
            continue
        if name[0] == "m" and not scaled:
            scaled = True
            run_scales(parts_of("s")[0])
        dict(m=run_m, o=run_o, f=run_f, g=run_g, d=run_d, e=run_e)[name[0]](*name[1:])
    for c in started.values():
        c.wait_send()


def placed_row(values, width):
    at = lax.rem(lax.axis_index("fs") * width, 128)
    row = lax.dynamic_update_slice(jnp.zeros((256,), F32), values, (at,))
    return row[:128] + row[128:]


def local(
    tokens, mix_gain, out_gate_w, in_gate_w, value_w, out_gate_scale, in_gate_scale, value_scale, mix_taps, conv_gain,
    out_proj_w, proj_scale, ffn_gain, gate_w, up_w, gate_scale, up_scale, gate_taps, up_taps, gate_bias, up_bias, down_w, down_scale,
):
    pieces = []
    for c in range(4):
        pieces += [w[:, c * 128 : c * 128 + 128] for w in (out_gate_w, in_gate_w, value_w)]
    pieces.append((out_proj_w * proj_scale).T)
    for j in range(11):
        pieces += [w[:, j * 128 : j * 128 + 128] for w in (gate_w, up_w)]
    pieces.append((down_w * down_scale).T)
    own = jnp.concatenate([p.astype(BF) for p in pieces], axis=1)
    rows = [placed_row(v, 16) for v in (out_gate_scale, in_gate_scale, value_scale)]
    rows += [placed_row(v, 44) for v in (gate_scale, up_scale)] + [jnp.zeros((128,), F32)] * 3
    sown = jnp.stack(rows)
    n = len(PARTS)
    hbm, vmem = pl.BlockSpec(memory_space=pl.ANY), pl.BlockSpec(memory_space=pltpu.VMEM)
    bufs = [
        pltpu.VMEM((2, 4, 4, 8, 128), F32) if kind == "s" else pltpu.VMEM((2, 4, 4, 64, blocks * 128), BF)
        for kind, blocks, _ in PARTS
    ]
    dma = pltpu.SemaphoreType.DMA
    return pl.pallas_call(
        kernel,
        out_shape=jax.ShapeDtypeStruct((1, 512, 2048), BF),
        in_specs=[hbm, hbm, hbm] + [vmem] * 8,
        out_specs=hbm,
        scratch_shapes=bufs
        + [
            pltpu.VMEM((1024, 2048), BF),
            pltpu.VMEM((1024, 2048), BF),
            pltpu.VMEM((1024, 512), BF),
            pltpu.VMEM((1024, 128), F32),
            pltpu.VMEM((1024, 128), F32),
            pltpu.VMEM((1024, 2048), BF),
            pltpu.VMEM((1024, 2048), BF),
            pltpu.VMEM((1024, 1408), BF),
            pltpu.VMEM((1024, 2048), F32),
            pltpu.VMEM((512, 2048), BF),
            pltpu.VMEM((8, 1408), F32),
            dma((n, 5, 2)),
            dma((n, 5, 2)),
            dma((n + 1,)),
            dma((8,)),
            dma((8,)),
        ],
        compiler_params=pltpu.CompilerParams(collective_id=0, has_side_effects=True, vmem_limit_bytes=67043328),
        name="layer",
    )(
        tokens, own, sown, mix_gain[None], mix_taps, conv_gain[None], ffn_gain[None],
        gate_taps, up_taps, gate_bias[None], up_bias[None],
    )


def solution(mesh):
    placed = (
        P(("rep", "fs"), "tp", None),
        P(),
        P("fs", "tp"),
        P("fs", "tp"),
        P("fs", "tp"),
        P(("tp", "fs")),
        P(("tp", "fs")),
        P(("tp", "fs")),
        P(None, "tp"),
        P("tp"),
        P("tp", "fs"),
        P("fs"),
        P(),
        P("fs", "tp"),
        P("fs", "tp"),
        P(("tp", "fs")),
        P(("tp", "fs")),
        P(None, "tp"),
        P(None, "tp"),
        P("tp"),
        P("tp"),
        P("tp", "fs"),
        P("fs"),
    )
    return jax.shard_map(
        local, mesh=mesh, in_specs=placed, out_specs=P(("rep", "fs"), "tp", None), check_vma=False
    )
```

```python
import jax
import jax.numpy as jnp
from jax import lax
from jax.experimental import pallas as pl
from jax.experimental.pallas import tpu as pltpu
from jax.sharding import PartitionSpec as P

EPS = 1e-06
MESH = pl.DeviceIdType.MESH
BF, F32 = jnp.bfloat16, jnp.float32
RATE = 46.65e3
TM = 1024

PARTS = (
    ("s", 0, "xyz"),
    ("m", 3, "yxz"),
    ("m", 3, "xyz"),
    ("m", 3, "yxz"),
    ("m", 3, "zyx"),
    ("o", 4, "xyz"),
    ("g", 4, "yzx"),
    ("g", 2, "yxz"),
    ("g", 2, "yxz"),
    ("g", 6, "xzy"),
    ("g", 4, "zyx"),
    ("g", 4, "xyz"),
    ("d", 4, "xzy"),
    ("d", 2, "yzx"),
    ("d", 3, "xzy"),
    ("d", 2, "yzx"),
)


class Copy:
    def __init__(self, part, stage, axis, sign, spec, rows, deps, nbytes):
        self.part, self.stage, self.axis, self.sign = part, stage, axis, sign
        self.spec, self.rows, self.deps, self.nbytes = spec, rows, deps, nbytes
        self.key = (part, stage, 0 if sign > 0 else 1)


def copies_of(part, kind, blocks, order):
    have = dict(x="own", y="own", z="own")
    size = dict(x=4, y=4, z=2)
    row = 512 if kind == "s" else blocks * 256
    whole, halves = ((0, 8), ((0, 8), None)) if kind == "s" else ((0, 64), ((0, 32), (32, 32)))
    made, stage, before = [], 0, []

    def add(stage, axis, sign, spec, rows, deps):
        count = 1
        for a in "xyz":
            count *= size[a] if spec[a] == "all" else 1
        made.append(Copy(part, stage, axis, sign, dict(spec), rows, list(deps), count * rows[1] * row))
        return made[-1].key

    for axis in order:
        done = []
        if axis == "z":
            for sign, rows in zip((1, -1), halves):
                if rows:
                    done.append(add(stage, axis, sign, have, rows, before))
            stage += 1
        else:
            firsts = [add(stage, axis, sign, have, whole, before) for sign in (1, -1)]
            done += firsts
            for sign, first, rows in zip((1, -1), firsts, halves):
                if rows:
                    done.append(add(stage + 1, axis, sign, {**have, axis: -sign}, rows, before + [first]))
            stage += 2
        before = before + done
        have[axis] = "all"
    return made, before


def plan(segments, backlog=5.0, latency=2.4, issue=0.06, start=2.0):
    todo, ends = [], []
    for p, (kind, blocks, order) in enumerate(PARTS):
        made, end = copies_of(p, kind, blocks, order)
        todo += made
        ends.append(end)
    arrive, link = {}, {(a, s): 0.0 for a in "xyz" for s in (1, -1)}
    out, now, seg = [], start, 0
    while todo or seg < len(segments):
        moved = True
        while moved:
            moved = False
            for op in todo:
                if all(arrive.get(d, 1e9) <= now for d in op.deps) and link[op.axis, op.sign] - now < backlog:
                    link[op.axis, op.sign] = max(now, link[op.axis, op.sign]) + op.nbytes / RATE
                    arrive[op.key] = link[op.axis, op.sign] + latency
                    out.append(("send", op, now))
                    now += issue
                    todo.remove(op)
                    moved = True
                    break
        if seg < len(segments):
            name, us, needs = segments[seg]
            if all(arrive.get(k, 1e9) <= now for p in needs for k in ends[p]):
                out.append(("run", segments[seg], now))
                now += us
                seg += 1
                continue
        later = [v for v in arrive.values() if v > now]
        later += [v - backlog + 1e-6 for v in link.values() if v - backlog + 1e-6 > now]
        if not later:
            break
        now = min(later)
    return out, ends


def parts_of(kind):
    return [p for p, part in enumerate(PARTS) if part[0] == kind]


def homes():
    home, wide = [], []
    for kind, blocks, _ in PARTS:
        if kind == "m" and wide and wide[-1] == 384:
            home.append((len(wide) - 1, 384))
            wide[-1] = 768
        else:
            home.append((len(wide), 0))
            wide.append(blocks * 128 if kind != "s" else 0)
    return home, wide


def segments_of():
    out = [("norm", 2.4, [])]
    m = parts_of("m")
    for c in range(2):
        out.append((("m", c, m[2 * c]), 3.3, m[2 * c : 2 * c + 2] + parts_of("s")))
    out += [(("o",), 2.4, parts_of("o"))]
    out += [(("f", i), 1.1 if i else 2.8, []) for i in range(4)]
    j = 0
    for p in parts_of("g"):
        for b in range(PARTS[p][1] // 2):
            out.append((("g", j, p, b), 1.45, [p]))
            j += 1
    d = parts_of("d")
    k = 0
    for i, p in enumerate(d[:-1]):
        out += [(("d", p, k, i == 0), PARTS[p][1] * 0.57, [p])]
        k += PARTS[p][1] * 128
    out += [(("e", d[-1], k), 5.5 + PARTS[d[-1]][1] * 0.6, d[-1:])]
    return out


def dot_nt(a, b):
    return lax.dot_general(a, b, (((1,), (1,)), ((), ())), preferred_element_type=F32)


def shifted_sum(prev, cur, taps):
    both = jnp.concatenate([prev, cur], axis=0)
    one = pltpu.roll(both, 1, 0)[8:]
    two = pltpu.roll(both, 2, 0)[8:]
    return taps[2:3] * cur + taps[1:2] * one + taps[0:1] * two


def kernel(*refs):
    n = len(PARTS)
    (tok, wo, wi, wv, wp, wg, wu, wd, s_o, s_i, s_v, s_g, s_u, s_p, s_d) = refs[:15]
    (mixg, mtaps, cgain, fgain, gtaps, utaps, gbias, ubias, out) = refs[15:24]
    home, wide = homes()
    nb = len(wide)
    bufs = refs[24 : 24 + nb]
    (tt, xx, cc, ss, ssr, ps, pr, hh, yy, dr, sc, wf, sf, ssem, rsem, lsem, tsem, trsem) = refs[24 + nb :]
    rep, fs, tp = lax.axis_index("rep"), lax.axis_index("fs"), lax.axis_index("tp")
    z, y, x = fs // 16, lax.rem(fs // 4, 4), lax.rem(fs, 4)
    pos = dict(x=x, y=y, z=z)
    mate = (rep, fs, 1 - tp)

    def beside(axis, sign):
        if axis == "x":
            return (rep, z * 16 + y * 4 + lax.rem(x + sign + 4, 4), tp)
        if axis == "y":
            return (rep, z * 16 + lax.rem(y + sign + 4, 4) * 4 + x, tp)
        far = lax.rem(rep * 2 + z + sign + 4, 4)
        return (far // 2, lax.rem(far, 2) * 16 + y * 4 + x, tp)

    local, at = [], 0
    for w in (wo, wi, wv, wp, wg, wu, wd):
        local.append(pltpu.make_async_copy(w, wf.at[:, pl.ds(at, w.shape[1])], lsem.at[len(local)]))
        at += w.shape[1]
    mine = pl.multiple_of(tp * 512, 512)
    other = pl.multiple_of((1 - tp) * 512, 512)
    local.append(pltpu.make_async_copy(tok.at[0], tt.at[pl.ds(mine, 512)], lsem.at[len(local)]))
    for c in local:
        c.start()

    barrier = pltpu.get_barrier_semaphore()
    for axis in "xyz":
        for sign in (1, -1):
            pl.semaphore_signal(barrier, inc=1, device_id=beside(axis, sign), device_id_type=MESH)
    pl.semaphore_signal(barrier, inc=1, device_id=mate, device_id_type=MESH)

    for c in local[:-1]:
        c.wait()
    eye = lax.broadcasted_iota(jnp.int32, (64, 64), 0) == lax.broadcasted_iota(jnp.int32, (64, 64), 1)
    p_col, d_col = (jnp.sum(jnp.where(eye, v[...], 0.0), axis=1, keepdims=True) for v in (s_p, s_d))
    last = {}
    for p, (kind, blocks, _) in enumerate(PARTS):
        first = last.get(kind, 0)
        last[kind] = first + blocks
        if kind == "s":
            sf[...] = jnp.zeros((16, 128), F32)
            for k, v in enumerate((s_o, s_i, s_v)):
                sf[k : k + 1, 0:16] = v[...]
            for k, v in enumerate((s_g, s_u)):
                sf[11 + k : 12 + k, 0:44] = v[...]
            low = pltpu.roll(sf[0:8, :], lax.rem(fs * 16, 128), 1)
            high = pltpu.roll(sf[8:16, :], lax.rem(fs * 44, 128), 1)
            bufs[home[p][0]][z, y, x] = low + high
            continue
        for b in range(blocks):
            j = first + b
            if kind == "m":
                v = wf[:, pl.ds((j % 3) * 512 + j // 3 * 128, 128)]
            elif kind == "o":
                v = wf[:, pl.ds(1536 + j * 128, 128)] * p_col
            elif kind == "g":
                v = wf[:, pl.ds(2048 + (j % 2) * 1408 + j // 2 * 128, 128)]
            else:
                v = wf[:, pl.ds(2048 + 2816 + j * 128, 128)] * d_col
            at = home[p][1] + b * 128
            bufs[home[p][0]][z, y, x, :, at : at + 128] = v.astype(BF)
    pl.semaphore_wait(barrier, 7)

    def to_mate(src, dst, k):
        return pltpu.make_async_remote_copy(
            src_ref=src, dst_ref=dst, send_sem=tsem.at[k], recv_sem=trsem.at[k], device_id=mate, device_id_type=MESH
        )

    tokens_over = to_mate(tok.at[0], tt.at[pl.ds(mine, 512)], 0)
    tokens_over.start()
    local[-1].wait()

    def where(spec, axis):
        v = spec[axis]
        if v == "all":
            return pl.ds(0, 2 if axis == "z" else 4)
        if v == "own":
            return pl.ds(pos[axis], 1)
        return pl.ds(lax.rem(pos[axis] + v + 4, 4), 1)

    def rows_of(i, size):
        return pl.ds(pl.multiple_of(i * size, size), size)

    def whole(p, cols):
        return bufs[home[p][0]][:, :, :, :, cols].reshape(2048, -1)

    def run_norm():
        tokens_over.wait()

        @pl.loop(0, 1024 // 64)
        def _(i):
            r = rows_of(i, 64)
            v = tt[r, :].astype(F32)
            v = v * lax.rsqrt(jnp.mean(v * v, axis=1, keepdims=True) + EPS) * mixg[...]
            xx[r, :] = v.astype(BF)

    def run_scales(p):
        lane = lax.broadcasted_iota(jnp.int32, (1, 128), 1)
        for k in range(3):
            for b in range(4):
                total = None
                for d in range(8 * b, 8 * b + 8):
                    v = bufs[home[p][0]][d // 16, d // 4 % 4, d % 4, k : k + 1, :]
                    total = v if total is None else total + v
                sc[k : k + 1, b * 128 : b * 128 + 128] = total
        for k in range(3, 5):
            for b in range(11):
                total = jnp.zeros((1, 128), F32)
                for d in range(32):
                    low, high = max(44 * d - 128 * b, 0), min(44 * d + 44 - 128 * b, 128)
                    if low < high:
                        v = bufs[home[p][0]][d // 16, d // 4 % 4, d % 4, k : k + 1, :]
                        total = jnp.where((lane >= low) & (lane < high), v, total)
                sc[k : k + 1, b * 128 : b * 128 + 128] = total

    def run_m(c, p):
        consts = []
        for h in range(2):
            cols = slice(c * 256 + h * 128, c * 256 + h * 128 + 128)
            consts.append((cols, mtaps[:, cols] * (sc[0:1, cols] * sc[1:2, cols] * sc[2:3, cols]), cgain[:, cols]))

        def tile(i, prev):
            r = rows_of(i, TM)
            acc = jnp.dot(xx[r, :], whole(p, slice(None)), preferred_element_type=F32)
            kept = []
            for h, (cols, taps, gain) in enumerate(consts):
                at = h * 384
                cur = acc[:, at + 128 : at + 256] * acc[:, at + 256 : at + 384]
                conv = acc[:, at : at + 128] * shifted_sum(prev[h], cur, taps)
                if c + h == 0:
                    ss[r, :] = conv * conv
                else:
                    ss[r, :] += conv * conv
                cc[r, cols] = (conv * gain).astype(BF)
                kept.append(cur[TM - 8 :])
            return tuple(kept)

        zero = jnp.zeros((8, 128), F32)
        lax.fori_loop(0, 1024 // TM, tile, (zero, zero))

    def p_over(q):
        c = pl.ds(q * 512, 512)
        return to_mate(ps.at[:, c], pr.at[:, c], 2 + q)

    squares_over = to_mate(ss, ssr, 1)

    def eighths(p, q):
        return bufs[home[p][0]][q // 2, pl.ds(q % 2 * 2, 2)].reshape(512, -1)

    def run_o():
        (p,) = parts_of("o")
        squares_over.start()
        for q in range(4):
            ps[:, q * 512 : q * 512 + 512] = dot_nt(cc[...], eighths(p, q)).astype(BF)
            if q:
                p_over(q - 1).start()
        p_over(3).start()

    def run_f(i):
        if i == 0:
            squares_over.wait()
            for q in range(4):
                p_over(q).wait()

        @pl.loop(i * 4, i * 4 + 4)
        def _(k):
            r = rows_of(k, 64)
            row = lax.rsqrt(jnp.sum(ss[r, :] + ssr[r, :], axis=1, keepdims=True) * (1.0 / 1024) + EPS)
            v = tt[r, :].astype(F32) + row * (ps[r, :].astype(F32) + pr[r, :].astype(F32))
            b = v.astype(BF)
            tt[r, :] = b
            v = b.astype(F32)
            v = v * lax.rsqrt(jnp.mean(v * v, axis=1, keepdims=True) + EPS) * fgain[...]
            xx[r, :] = v.astype(BF)

    def run_g(j, p, b):
        cols = slice(j * 128, j * 128 + 128)
        tg, tu, bg, bu = gtaps[:, cols], utaps[:, cols], gbias[:, cols], ubias[:, cols]
        sg, su = sc[3:4, cols], sc[4:5, cols]

        tg, tu = tg * sg, tu * su

        def tile(i, prev):
            r = rows_of(i, TM)
            acc = jnp.dot(xx[r, :], whole(p, slice(b * 256, b * 256 + 256)), preferred_element_type=F32)
            g, u = acc[:, :128], acc[:, 128:]
            ga = shifted_sum(prev[0], g, tg) + bg
            ua = shifted_sum(prev[1], u, tu) + bu
            hh[r, cols] = (ga / (1.0 + jnp.exp(-ga)) * ua).astype(BF)
            return g[TM - 8 :], u[TM - 8 :]

        zero = jnp.zeros((8, 128), F32)
        lax.fori_loop(0, 1024 // TM, tile, (zero, zero))

    def run_d(p, k, first):
        for q in range(4):
            w = eighths(p, q)
            v = dot_nt(hh[:, k : k + w.shape[1]], w)
            c = slice(q * 512, q * 512 + 512)
            yy[0:1024, c] = v if first else yy[0:1024, c] + v

    def d_over(q):
        c = pl.ds(q * 512, 512)
        return to_mate(ps.at[pl.ds(0, 512), c], dr.at[:, c], 6 + q)

    def run_e(p, k):
        own, far = pl.ds(mine, 512), pl.ds(other, 512)
        for q in range(4):
            w = eighths(p, q)
            c = slice(q * 512, q * 512 + 512)
            ps[0:512, c] = (yy[far, c] + dot_nt(hh[far, k : k + w.shape[1]], w)).astype(BF)
            if q:
                d_over(q - 1).start()
        d_over(3).start()
        written = []
        for q in range(4):
            w = eighths(p, q)
            c = slice(q * 512, q * 512 + 512)
            yy[own, c] += dot_nt(hh[own, k : k + w.shape[1]], w)
            d_over(q).wait()

            @pl.loop(0, 8)
            def _(i):
                r = pl.ds(pl.multiple_of(mine + i * 64, 64), 64)
                o = rows_of(i, 64)
                xx[o, c] = (tt[r, c].astype(F32) + yy[r, c] + dr[o, c].astype(F32)).astype(BF)

            w = pltpu.make_async_copy(xx.at[pl.ds(0, 512), pl.ds(q * 512, 512)], out.at[0, :, pl.ds(q * 512, 512)], lsem.at[q])
            w.start()
            written.append(w)
        for w in written:
            w.wait()

    steps, ends = plan(segments_of())
    started, got = {}, set()

    def arrived(keys):
        for key in keys:
            if key not in got:
                got.add(key)
                started[key].wait_recv()

    scaled = False
    for what, it, _ in steps:
        if what == "send":
            arrived(it.deps)
            kind, blocks, _ = PARTS[it.part]
            b, at = home[it.part]
            ref = bufs[b].at[where(it.spec, "z"), where(it.spec, "y"), where(it.spec, "x"), pl.ds(*it.rows), pl.ds(at, max(blocks, 1) * 128)]
            c = pltpu.make_async_remote_copy(
                src_ref=ref,
                dst_ref=ref,
                send_sem=ssem.at[it.key],
                recv_sem=rsem.at[it.key],
                device_id=beside(it.axis, it.sign),
                device_id_type=MESH,
            )
            c.start()
            started[it.key] = c
            continue
        name, _, needs = it
        for p in needs:
            arrived(ends[p])
        if name == "norm":
            run_norm()
            continue
        if name[0] == "m" and not scaled:
            scaled = True
            run_scales(parts_of("s")[0])
        dict(m=run_m, o=run_o, f=run_f, g=run_g, d=run_d, e=run_e)[name[0]](*name[1:])
    for c in started.values():
        c.wait_send()


def local(
    tokens, mix_gain, out_gate_w, in_gate_w, value_w, out_gate_scale, in_gate_scale, value_scale, mix_taps, conv_gain,
    out_proj_w, proj_scale, ffn_gain, gate_w, up_w, gate_scale, up_scale, gate_taps, up_taps, gate_bias, up_bias, down_w, down_scale,
):
    n = len(PARTS)
    hbm, vmem = pl.BlockSpec(memory_space=pl.ANY), pl.BlockSpec(memory_space=pltpu.VMEM)
    bufs = [pltpu.VMEM((2, 4, 4, 64, w), BF) if w else pltpu.VMEM((2, 4, 4, 8, 128), F32) for w in homes()[1]]
    dma = pltpu.SemaphoreType.DMA
    return pl.pallas_call(
        kernel,
        out_shape=jax.ShapeDtypeStruct((1, 512, 2048), BF),
        in_specs=[hbm] * 8 + [vmem] * 15,
        out_specs=hbm,
        scratch_shapes=bufs
        + [
            pltpu.VMEM((1024, 2048), BF),
            pltpu.VMEM((1024, 2048), BF),
            pltpu.VMEM((1024, 512), BF),
            pltpu.VMEM((1024, 128), F32),
            pltpu.VMEM((1024, 128), F32),
            pltpu.VMEM((1024, 2048), BF),
            pltpu.VMEM((1024, 2048), BF),
            pltpu.VMEM((1024, 1408), BF),
            pltpu.VMEM((1024, 2048), F32),
            pltpu.VMEM((512, 2048), BF),
            pltpu.VMEM((8, 1408), F32),
            pltpu.VMEM((64, 6272), F32),
            pltpu.VMEM((16, 128), F32),
            dma((n, 5, 2)),
            dma((n, 5, 2)),
            dma((8,)),
            dma((10,)),
            dma((10,)),
        ],
        compiler_params=pltpu.CompilerParams(collective_id=0, has_side_effects=True, vmem_limit_bytes=67043328),
        name="layer",
    )(
        tokens, out_gate_w, in_gate_w, value_w, out_proj_w.T, gate_w, up_w, down_w.T,
        out_gate_scale[None], in_gate_scale[None], value_scale[None], gate_scale[None], up_scale[None],
        proj_scale[None], down_scale[None], mix_gain[None], mix_taps, conv_gain[None], ffn_gain[None],
        gate_taps, up_taps, gate_bias[None], up_bias[None],
    )


def solution(mesh):
    placed = (
        P(("rep", "fs"), "tp", None),
        P(),
        P("fs", "tp"),
        P("fs", "tp"),
        P("fs", "tp"),
        P(("tp", "fs")),
        P(("tp", "fs")),
        P(("tp", "fs")),
        P(None, "tp"),
        P("tp"),
        P("tp", "fs"),
        P("fs"),
        P(),
        P("fs", "tp"),
        P("fs", "tp"),
        P(("tp", "fs")),
        P(("tp", "fs")),
        P(None, "tp"),
        P(None, "tp"),
        P("tp"),
        P("tp"),
        P("tp", "fs"),
        P("fs"),
    )
    return jax.shard_map(
        local, mesh=mesh, in_specs=placed, out_specs=P(("rep", "fs"), "tp", None), check_vma=False
    )
```

```python
import jax
import jax.numpy as jnp
from jax import lax
from jax.experimental import pallas as pl
from jax.experimental.pallas import tpu as pltpu
from jax.sharding import PartitionSpec as P

EPS = 1e-06
MESH = pl.DeviceIdType.MESH
BF, F32 = jnp.bfloat16, jnp.float32
RATE = 46.65e3
TM = 1024

PARTS = (
    ("s", 0, "xyz"),
    ("m", 3, "yxz"),
    ("m", 3, "xyz"),
    ("m", 3, "xzy"),
    ("m", 3, "xzy"),
    ("o", 4, "yxz"),
    ("g", 2, "zyx"),
    ("g", 2, "yzx"),
    ("g", 4, "xyz"),
    ("g", 4, "xyz"),
    ("g", 6, "yzx"),
    ("g", 2, "xyz"),
    ("g", 2, "zxy"),
    ("d", 2, "xyz"),
    ("d", 2, "xzy"),
    ("d", 4, "zyx"),
    ("d", 3, "yzx"),
)


class Copy:
    def __init__(self, part, stage, axis, sign, spec, rows, deps, nbytes):
        self.part, self.stage, self.axis, self.sign = part, stage, axis, sign
        self.spec, self.rows, self.deps, self.nbytes = spec, rows, deps, nbytes
        self.key = (part, stage, 0 if sign > 0 else 1)


def copies_of(part, kind, blocks, order):
    have = dict(x="own", y="own", z="own")
    size = dict(x=4, y=4, z=2)
    row = 512 if kind == "s" else blocks * 256
    whole, halves = ((0, 8), ((0, 8), None)) if kind == "s" else ((0, 64), ((0, 32), (32, 32)))
    made, stage, before = [], 0, []

    def add(stage, axis, sign, spec, rows, deps):
        count = 1
        for a in "xyz":
            count *= size[a] if spec[a] == "all" else 1
        made.append(Copy(part, stage, axis, sign, dict(spec), rows, list(deps), count * rows[1] * row))
        return made[-1].key

    for axis in order:
        done = []
        if axis == "z":
            for sign, rows in zip((1, -1), halves):
                if rows:
                    done.append(add(stage, axis, sign, have, rows, before))
            stage += 1
        else:
            firsts = [add(stage, axis, sign, have, whole, before) for sign in (1, -1)]
            done += firsts
            for sign, first, rows in zip((1, -1), firsts, halves):
                if rows:
                    done.append(add(stage + 1, axis, sign, {**have, axis: -sign}, rows, before + [first]))
            stage += 2
        before = before + done
        have[axis] = "all"
    return made, before


def plan(segments, backlog=5.0, spare=2.0, window=1, latency=2.6, issue=0.12, start=9.0, slower=1.2):
    todo, ends = [], []
    for p, (kind, blocks, order) in enumerate(PARTS):
        made, end = copies_of(p, kind, blocks, order)
        for op in made:
            if op.stage == 0 and kind in "ogd":
                op.deps.append(("cast", kind))
        todo += made
        ends.append(end)
    arrive, link = {}, {(a, s): 0.0 for a in "xyz" for s in (1, -1)}
    out, now, seg = [], start, 0
    while todo or seg < len(segments):
        moved, ready = True, False
        if seg < len(segments):
            name, us, needs = segments[seg]
            us *= slower
            ready = all(arrive.get(k, 1e9) <= now for p in needs for k in ends[p])
        while moved:
            moved = False
            front = min((op.part for op in todo), default=0)
            for op in todo:
                limit = (backlog if op.part - front < window else spare) + (us if ready else 0.0)
                if all(arrive.get(d, 1e9) <= now for d in op.deps) and link[op.axis, op.sign] - now < limit:
                    link[op.axis, op.sign] = max(now, link[op.axis, op.sign]) + op.nbytes / RATE
                    arrive[op.key] = link[op.axis, op.sign] + latency
                    out.append(("send", op, now))
                    now += issue
                    todo.remove(op)
                    moved = True
                    break
        if ready:
            out.append(("run", segments[seg], now))
            now += us
            arrive[name] = now
            seg += 1
            continue
        later = [v for v in arrive.values() if v > now]
        later += [v - b + 1e-6 for v in link.values() for b in (backlog, spare) if v - b + 1e-6 > now]
        if not later:
            break
        now = min(later)
    return out, ends


def parts_of(kind):
    return [p for p, part in enumerate(PARTS) if part[0] == kind]


def homes():
    home, wide = [], []
    for kind, blocks, _ in PARTS:
        if kind == "m" and wide and wide[-1] == 384:
            home.append((len(wide) - 1, 384))
            wide[-1] = 768
        else:
            home.append((len(wide), 0))
            wide.append(blocks * 128 if kind != "s" else 0)
    return home, wide


def segments_of():
    out = [(("cast", k), 0.4, []) for k in "ogd"] + [(("norm", h), 0.6, []) for h in range(4)]
    m = parts_of("m")
    for c in range(2):
        out.append((("m", c, m[2 * c]), 3.3, m[2 * c : 2 * c + 2] + parts_of("s")))
    out += [(("o", q), 0.6, parts_of("o")) for q in range(4)]
    out += [(("f", i), 1.1 if i else 2.8, []) for i in range(4)]
    j = 0
    for p in parts_of("g"):
        for b in range(PARTS[p][1] // 2):
            out.append((("g", j, p, b), 1.45, [p]))
            j += 1
    d = parts_of("d")
    k = 0
    for i, p in enumerate(d[:-1]):
        out += [(("d", p, k, i == 0, q), 0.25 + PARTS[p][1] * 0.08, [p]) for q in range(4)]
        k += PARTS[p][1] * 128
    out += [(("e", d[-1], k), 6.0 + PARTS[d[-1]][1] * 0.4, d[-1:])]
    return out


def dot_nt(a, b):
    return lax.dot_general(a, b, (((1,), (1,)), ((), ())), preferred_element_type=F32)


def shifted_sum(prev, cur, taps):
    both = jnp.concatenate([prev, cur], axis=0)
    one = pltpu.roll(both, 1, 0)[8:]
    two = pltpu.roll(both, 2, 0)[8:]
    return taps[2:3] * cur + taps[1:2] * one + taps[0:1] * two


def kernel(*refs):
    n = len(PARTS)
    (tok, wo, wi, wv, wp, wg, wu, wd, s_o, s_i, s_v, s_g, s_u, s_p, s_d) = refs[:15]
    (mixg, mtaps, cgain, fgain, gtaps, utaps, gbias, ubias, out) = refs[15:24]
    home, wide = homes()
    nb = len(wide)
    bufs = refs[24 : 24 + nb]
    (tt, xx, cc, ss, ssr, ps, pr, hh, yy, sc, wf, sf, credit, ssem, rsem, lsem, tsem, trsem) = refs[24 + nb :]
    rep, fs, tp = lax.axis_index("rep"), lax.axis_index("fs"), lax.axis_index("tp")
    z, y, x = fs // 16, lax.rem(fs // 4, 4), lax.rem(fs, 4)
    pos = dict(x=x, y=y, z=z)
    mate = (rep, fs, 1 - tp)

    def beside(axis, sign):
        if axis == "x":
            return (rep, z * 16 + y * 4 + lax.rem(x + sign + 4, 4), tp)
        if axis == "y":
            return (rep, z * 16 + lax.rem(y + sign + 4, 4) * 4 + x, tp)
        far = lax.rem(rep * 2 + z + sign + 4, 4)
        return (far // 2, lax.rem(far, 2) * 16 + y * 4 + x, tp)

    local, at = [], 0
    for w in (wo, wi, wv, wp, wg, wu, wd):
        local.append(pltpu.make_async_copy(w, wf.at[:, pl.ds(at, w.shape[1])], lsem.at[len(local)]))
        at += w.shape[1]
    mine = pl.multiple_of(tp * 512, 512)
    other = pl.multiple_of((1 - tp) * 512, 512)
    local.append(pltpu.make_async_copy(tok.at[0], tt.at[pl.ds(mine, 512)], lsem.at[len(local)]))
    for c in local:
        c.start()

    barrier = pltpu.get_barrier_semaphore()
    for axis in "xyz":
        for sign in (1, -1):
            pl.semaphore_signal(barrier, inc=1, device_id=beside(axis, sign), device_id_type=MESH)
    pl.semaphore_signal(barrier, inc=1, device_id=mate, device_id_type=MESH)

    def cast(kind):
        for i in dict(m=(0, 1, 2), o=(3,), g=(4, 5), d=(6,), s=())[kind]:
            local[i].wait()
        if kind == "s":
            sf[...] = jnp.zeros((16, 128), F32)
            for k, v in enumerate((s_o, s_i, s_v)):
                sf[k : k + 1, 0:16] = v[...]
            for k, v in enumerate((s_g, s_u)):
                sf[11 + k : 12 + k, 0:44] = v[...]
            low = pltpu.roll(sf[0:8, :], lax.rem(fs * 16, 128), 1)
            high = pltpu.roll(sf[8:16, :], lax.rem(fs * 44, 128), 1)
            bufs[home[parts_of("s")[0]][0]][z, y, x] = low + high
            return
        column = None
        if kind in "od":
            eye = lax.broadcasted_iota(jnp.int32, (64, 64), 0) == lax.broadcasted_iota(jnp.int32, (64, 64), 1)
            column = jnp.sum(jnp.where(eye, (s_p if kind == "o" else s_d)[...], 0.0), axis=1, keepdims=True)
        j = 0
        for p in parts_of(kind):
            for b in range(PARTS[p][1]):
                if kind == "m":
                    v = wf[:, pl.ds((j % 3) * 512 + j // 3 * 128, 128)]
                elif kind == "g":
                    v = wf[:, pl.ds(2048 + (j % 2) * 1408 + j // 2 * 128, 128)]
                else:
                    v = wf[:, pl.ds((1536 if kind == "o" else 2048 + 2816) + j * 128, 128)] * column
                at = home[p][1] + b * 128
                bufs[home[p][0]][z, y, x, :, at : at + 128] = v.astype(BF)
                j += 1

    cast("s")
    cast("m")
    pl.semaphore_wait(barrier, 7)

    def to_mate(src, dst, k):
        return pltpu.make_async_remote_copy(
            src_ref=src, dst_ref=dst, send_sem=tsem.at[k], recv_sem=trsem.at[k], device_id=mate, device_id_type=MESH
        )

    tokens_over = to_mate(tok.at[0], tt.at[pl.ds(mine, 512)], 0)
    tokens_over.start()

    def where(spec, axis):
        v = spec[axis]
        if v == "all":
            return pl.ds(0, 2 if axis == "z" else 4)
        if v == "own":
            return pl.ds(pos[axis], 1)
        return pl.ds(lax.rem(pos[axis] + v + 4, 4), 1)

    def rows_of(i, size):
        return pl.ds(pl.multiple_of(i * size, size), size)

    def whole(p, cols):
        return bufs[home[p][0]][:, :, :, :, cols].reshape(2048, -1)

    def run_norm(h):
        if h == 0:
            local[-1].wait()
            tokens_over.wait()

        @pl.loop(h * 4, h * 4 + 4)
        def _(i):
            r = rows_of(i, 64)
            v = tt[r, :].astype(F32)
            v = v * lax.rsqrt(jnp.mean(v * v, axis=1, keepdims=True) + EPS) * mixg[...]
            xx[r, :] = v.astype(BF)

    def run_scales(p):
        lane = lax.broadcasted_iota(jnp.int32, (1, 128), 1)
        for k in range(3):
            for b in range(4):
                total = None
                for d in range(8 * b, 8 * b + 8):
                    v = bufs[home[p][0]][d // 16, d // 4 % 4, d % 4, k : k + 1, :]
                    total = v if total is None else total + v
                sc[k : k + 1, b * 128 : b * 128 + 128] = total
        for k in range(3, 5):
            for b in range(11):
                total = jnp.zeros((1, 128), F32)
                for d in range(32):
                    low, high = max(44 * d - 128 * b, 0), min(44 * d + 44 - 128 * b, 128)
                    if low < high:
                        v = bufs[home[p][0]][d // 16, d // 4 % 4, d % 4, k : k + 1, :]
                        total = jnp.where((lane >= low) & (lane < high), v, total)
                sc[k : k + 1, b * 128 : b * 128 + 128] = total

    def run_m(c, p):
        consts = []
        for h in range(2):
            cols = slice(c * 256 + h * 128, c * 256 + h * 128 + 128)
            consts.append((cols, mtaps[:, cols] * (sc[0:1, cols] * sc[1:2, cols] * sc[2:3, cols]), cgain[:, cols]))

        def tile(i, prev):
            r = rows_of(i, TM)
            acc = jnp.dot(xx[r, :], whole(p, slice(None)), preferred_element_type=F32)
            kept = []
            for h, (cols, taps, gain) in enumerate(consts):
                at = h * 384
                cur = acc[:, at + 128 : at + 256] * acc[:, at + 256 : at + 384]
                conv = acc[:, at : at + 128] * shifted_sum(prev[h], cur, taps)
                if c + h == 0:
                    ss[r, :] = conv * conv
                else:
                    ss[r, :] += conv * conv
                cc[r, cols] = (conv * gain).astype(BF)
                kept.append(cur[TM - 8 :])
            return tuple(kept)

        zero = jnp.zeros((8, 128), F32)
        lax.fori_loop(0, 1024 // TM, tile, (zero, zero))

    def p_over(q):
        c = pl.ds(q * 512, 512)
        return to_mate(ps.at[:, c], pr.at[:, c], 2 + q)

    squares_over = to_mate(ss, ssr, 1)

    def eighths(p, q):
        return bufs[home[p][0]][q // 2, pl.ds(q % 2 * 2, 2)].reshape(512, -1)

    def run_o(q):
        (p,) = parts_of("o")
        if q == 0:
            squares_over.start()
        ps[:, q * 512 : q * 512 + 512] = dot_nt(cc[...], eighths(p, q)).astype(BF)
        if q:
            p_over(q - 1).start()
        if q == 3:
            p_over(3).start()

    def run_f(i):
        if i == 0:
            squares_over.wait()
            for q in range(4):
                p_over(q).wait()

        @pl.loop(i * 4, i * 4 + 4)
        def _(k):
            r = rows_of(k, 64)
            row = lax.rsqrt(jnp.sum(ss[r, :] + ssr[r, :], axis=1, keepdims=True) * (1.0 / 1024) + EPS)
            v = tt[r, :].astype(F32) + row * (ps[r, :].astype(F32) + pr[r, :].astype(F32))
            b = v.astype(BF)
            tt[r, :] = b
            v = b.astype(F32)
            v = v * lax.rsqrt(jnp.mean(v * v, axis=1, keepdims=True) + EPS) * fgain[...]
            xx[r, :] = v.astype(BF)

        if i == 3:
            pl.semaphore_signal(credit, inc=1, device_id=mate, device_id_type=MESH)

    def run_g(j, p, b):
        cols = slice(j * 128, j * 128 + 128)
        tg, tu, bg, bu = gtaps[:, cols], utaps[:, cols], gbias[cols][None], ubias[cols][None]
        sg, su = sc[3:4, cols], sc[4:5, cols]

        tg, tu = tg * sg, tu * su

        def tile(i, prev):
            r = rows_of(i, TM)
            acc = jnp.dot(xx[r, :], whole(p, slice(b * 256, b * 256 + 256)), preferred_element_type=F32)
            g, u = acc[:, :128], acc[:, 128:]
            ga = shifted_sum(prev[0], g, tg) + bg
            ua = shifted_sum(prev[1], u, tu) + bu
            hh[r, cols] = (ga / (1.0 + jnp.exp(-ga)) * ua).astype(BF)
            return g[TM - 8 :], u[TM - 8 :]

        zero = jnp.zeros((8, 128), F32)
        lax.fori_loop(0, 1024 // TM, tile, (zero, zero))

    def run_d(p, k, first, q):
        w = eighths(p, q)
        v = dot_nt(hh[:, k : k + w.shape[1]], w)
        c = slice(q * 512, q * 512 + 512)
        yy[:, c] = v if first else yy[:, c] + v

    def d_over(q):
        c = pl.ds(q * 512, 512)
        return to_mate(ps.at[pl.ds(0, 512), c], pr.at[pl.ds(0, 512), c], 6 + q)

    def run_e(p, k):
        own, far = pl.ds(mine, 512), pl.ds(other, 512)
        for q in range(4):
            w = eighths(p, q)
            c = slice(q * 512, q * 512 + 512)
            ps[0:512, c] = (yy[far, c] + dot_nt(hh[far, k : k + w.shape[1]], w)).astype(BF)
            if q == 1:
                pl.semaphore_wait(credit, 1)
            if q:
                d_over(q - 1).start()
        d_over(3).start()
        for q in range(4):
            w = eighths(p, q)
            c = slice(q * 512, q * 512 + 512)
            yy[own, c] += dot_nt(hh[own, k : k + w.shape[1]], w)
            d_over(q).wait()

            @pl.loop(0, 8)
            def _(i):
                r = pl.ds(pl.multiple_of(mine + i * 64, 64), 64)
                o = rows_of(i, 64)
                out[0, o, c] = (tt[r, c].astype(F32) + yy[r, c] + pr[o, c].astype(F32)).astype(BF)

    steps, ends = plan(segments_of())
    started, got = {}, set()

    def arrived(keys):
        for key in keys:
            if key not in got and key[0] != "cast":
                got.add(key)
                started[key].wait_recv()

    scaled = False
    for what, it, _ in steps:
        if what == "send":
            arrived(it.deps)
            kind, blocks, _ = PARTS[it.part]
            b, at = home[it.part]
            ref = bufs[b].at[where(it.spec, "z"), where(it.spec, "y"), where(it.spec, "x"), pl.ds(*it.rows), pl.ds(at, max(blocks, 1) * 128)]
            c = pltpu.make_async_remote_copy(
                src_ref=ref,
                dst_ref=ref,
                send_sem=ssem.at[it.key],
                recv_sem=rsem.at[it.key],
                device_id=beside(it.axis, it.sign),
                device_id_type=MESH,
            )
            c.start()
            started[it.key] = c
            continue
        name, _, needs = it
        for p in needs:
            arrived(ends[p])
        if name[0] == "m" and not scaled:
            scaled = True
            run_scales(parts_of("s")[0])
        dict(cast=cast, norm=run_norm, m=run_m, o=run_o, f=run_f, g=run_g, d=run_d, e=run_e)[name[0]](*name[1:])
    for c in started.values():
        c.wait_send()


def local(
    tokens, mix_gain, out_gate_w, in_gate_w, value_w, out_gate_scale, in_gate_scale, value_scale, mix_taps, conv_gain,
    out_proj_w, proj_scale, ffn_gain, gate_w, up_w, gate_scale, up_scale, gate_taps, up_taps, gate_bias, up_bias, down_w, down_scale,
):
    n = len(PARTS)
    hbm, vmem = pl.BlockSpec(memory_space=pl.ANY), pl.BlockSpec(memory_space=pltpu.VMEM)
    bufs = [pltpu.VMEM((2, 4, 4, 64, w), BF) if w else pltpu.VMEM((2, 4, 4, 8, 128), F32) for w in homes()[1]]
    dma = pltpu.SemaphoreType.DMA
    return pl.pallas_call(
        kernel,
        out_shape=pltpu.VMEM((1, 512, 2048), BF),
        in_specs=[hbm] * 8 + [vmem] * 15,
        out_specs=vmem,
        scratch_shapes=bufs
        + [
            pltpu.VMEM((1024, 2048), BF),
            pltpu.VMEM((1024, 2048), BF),
            pltpu.VMEM((1024, 512), BF),
            pltpu.VMEM((1024, 128), F32),
            pltpu.VMEM((1024, 128), F32),
            pltpu.VMEM((1024, 2048), BF),
            pltpu.VMEM((1024, 2048), BF),
            pltpu.VMEM((1024, 1408), BF),
            pltpu.VMEM((1024, 2048), F32),
            pltpu.VMEM((8, 1408), F32),
            pltpu.VMEM((64, 6272), F32),
            pltpu.VMEM((16, 128), F32),
            pltpu.SemaphoreType.REGULAR,
            dma((n, 5, 2)),
            dma((n, 5, 2)),
            dma((8,)),
            dma((10,)),
            dma((10,)),
        ],
        compiler_params=pltpu.CompilerParams(collective_id=0, has_side_effects=True, vmem_limit_bytes=64600000),
        name="layer",
    )(
        tokens, out_gate_w, in_gate_w, value_w, out_proj_w.T, gate_w, up_w, down_w.T,
        out_gate_scale[None], in_gate_scale[None], value_scale[None], gate_scale[None], up_scale[None],
        proj_scale[None], down_scale[None], mix_gain[None], mix_taps, conv_gain[None], ffn_gain[None],
        gate_taps, up_taps, gate_bias, up_bias,
    )


def solution(mesh):
    placed = (
        P(("rep", "fs"), "tp", None),
        P(),
        P("fs", "tp"),
        P("fs", "tp"),
        P("fs", "tp"),
        P(("tp", "fs")),
        P(("tp", "fs")),
        P(("tp", "fs")),
        P(None, "tp"),
        P("tp"),
        P("tp", "fs"),
        P("fs"),
        P(),
        P("fs", "tp"),
        P("fs", "tp"),
        P(("tp", "fs")),
        P(("tp", "fs")),
        P(None, "tp"),
        P(None, "tp"),
        P("tp"),
        P("tp"),
        P("tp", "fs"),
        P("fs"),
    )
    return jax.shard_map(
        local, mesh=mesh, in_specs=placed, out_specs=P(("rep", "fs"), "tp", None), check_vma=False
    )
```

```python
import jax
import jax.numpy as jnp
from jax import lax
from jax.experimental import pallas as pl
from jax.experimental.pallas import tpu as pltpu
from jax.sharding import PartitionSpec as P

EPS = 1e-06
MESH = pl.DeviceIdType.MESH
BF, F32 = jnp.bfloat16, jnp.float32
RATE = 46.65e3
TM = 1024

PARTS = (
    ("s", 0, "xyz"),
    ("m", 3, "yxz"),
    ("m", 3, "xzy"),
    ("m", 3, "xyz"),
    ("m", 3, "yxz"),
    ("o", 4, "yzx"),
    ("g", 4, "xzy"),
    ("g", 2, "yxz"),
    ("g", 2, "xyz"),
    ("g", 4, "yxz"),
    ("g", 2, "zyx"),
    ("g", 2, "yzx"),
    ("g", 2, "yxz"),
    ("g", 4, "xzy"),
    ("d", 3, "xyz"),
    ("d", 2, "zxy"),
    ("d", 1, "xzy"),
    ("d", 3, "zyx"),
    ("d", 2, "zyx"),
)


class Copy:
    def __init__(self, part, stage, axis, sign, spec, rows, deps, nbytes):
        self.part, self.stage, self.axis, self.sign = part, stage, axis, sign
        self.spec, self.rows, self.deps, self.nbytes = spec, rows, deps, nbytes
        self.key = (part, stage, 0 if sign > 0 else 1)


def copies_of(part, kind, blocks, order):
    have = dict(x="own", y="own", z="own")
    size = dict(x=4, y=4, z=2)
    row = 512 if kind == "s" else blocks * 256
    whole, halves = ((0, 8), ((0, 8), None)) if kind == "s" else ((0, 64), ((0, 32), (32, 32)))
    made, stage, before = [], 0, []

    def add(stage, axis, sign, spec, rows, deps):
        count = 1
        for a in "xyz":
            count *= size[a] if spec[a] == "all" else 1
        made.append(Copy(part, stage, axis, sign, dict(spec), rows, list(deps), count * rows[1] * row))
        return made[-1].key

    for axis in order:
        done = []
        if axis == "z":
            for sign, rows in zip((1, -1), halves):
                if rows:
                    done.append(add(stage, axis, sign, have, rows, before))
            stage += 1
        else:
            firsts = [add(stage, axis, sign, have, whole, before) for sign in (1, -1)]
            done += firsts
            for sign, first, rows in zip((1, -1), firsts, halves):
                if rows:
                    done.append(add(stage + 1, axis, sign, {**have, axis: -sign}, rows, before + [first]))
            stage += 2
        before = before + done
        have[axis] = "all"
    return made, before


def plan(segments, backlog=4.0, spare=1.5, window=2, latency=2.6, issue=0.12, start=9.0, slower=1.2):
    todo, ends = [], []
    for p, (kind, blocks, order) in enumerate(PARTS):
        made, end = copies_of(p, kind, blocks, order)
        for op in made:
            if op.stage == 0 and kind in "ogd":
                op.deps.append(("cast", kind))
        todo += made
        ends.append(end)
    arrive, link = {}, {(a, s): 0.0 for a in "xyz" for s in (1, -1)}
    out, now, seg = [], start, 0
    while todo or seg < len(segments):
        moved, ready = True, False
        if seg < len(segments):
            name, us, needs = segments[seg]
            us *= slower
            ready = all(arrive.get(k, 1e9) <= now for p in needs for k in ends[p])
        while moved:
            moved = False
            front = min((op.part for op in todo), default=0)
            for op in todo:
                limit = (backlog if op.part - front < window else spare) + (us if ready else 0.0)
                if all(arrive.get(d, 1e9) <= now for d in op.deps) and link[op.axis, op.sign] - now < limit:
                    link[op.axis, op.sign] = max(now, link[op.axis, op.sign]) + op.nbytes / RATE
                    arrive[op.key] = link[op.axis, op.sign] + latency
                    out.append(("send", op, now))
                    now += issue
                    todo.remove(op)
                    moved = True
                    break
        if ready:
            out.append(("run", segments[seg], now))
            now += us
            arrive[name] = now
            seg += 1
            continue
        later = [v for v in arrive.values() if v > now]
        later += [v - b + 1e-6 for v in link.values() for b in (backlog, spare) if v - b + 1e-6 > now]
        if not later:
            break
        now = min(later)
    return out, ends


def parts_of(kind):
    return [p for p, part in enumerate(PARTS) if part[0] == kind]


def homes():
    home, wide = [], []
    for kind, blocks, _ in PARTS:
        if kind == "m" and wide and wide[-1] == 384:
            home.append((len(wide) - 1, 384))
            wide[-1] = 768
        else:
            home.append((len(wide), 0))
            wide.append(blocks * 128 if kind != "s" else 0)
    return home, wide


def segments_of():
    out = [(("cast", k), 0.4, []) for k in "ogd"] + [(("norm", h), 0.6, []) for h in range(4)]
    m = parts_of("m")
    for c in range(2):
        out.append((("m", c, m[2 * c]), 3.3, m[2 * c : 2 * c + 2] + parts_of("s")))
    out += [(("o", q), 0.6, parts_of("o")) for q in range(4)]
    out += [(("f", i), 1.1 if i else 2.8, []) for i in range(4)]
    j = 0
    for p in parts_of("g"):
        for b in range(PARTS[p][1] // 2):
            out.append((("g", j, p, b), 1.45, [p]))
            j += 1
    d = parts_of("d")
    k = 0
    for i, p in enumerate(d[:-1]):
        out += [(("d", p, k, i == 0, q), 0.25 + PARTS[p][1] * 0.08, [p]) for q in range(4)]
        k += PARTS[p][1] * 128
    out += [(("e", d[-1], k), 6.0 + PARTS[d[-1]][1] * 0.4, d[-1:])]
    return out


def dot_nt(a, b):
    return lax.dot_general(a, b, (((1,), (1,)), ((), ())), preferred_element_type=F32)


def shifted_sum(prev, cur, taps):
    both = jnp.concatenate([prev, cur], axis=0)
    one = pltpu.roll(both, 1, 0)[8:]
    two = pltpu.roll(both, 2, 0)[8:]
    return taps[2:3] * cur + taps[1:2] * one + taps[0:1] * two


def kernel(*refs):
    n = len(PARTS)
    (tok, wo, wi, wv, wp, wg, wu, wd, s_o, s_i, s_v, s_g, s_u, s_p, s_d) = refs[:15]
    (mixg, mtaps, cgain, fgain, gtaps, utaps, gbias, ubias, out) = refs[15:24]
    home, wide = homes()
    nb = len(wide)
    bufs = refs[24 : 24 + nb]
    (tt, xx, cc, ss, ssr, ps, pr, hh, yy, sc, wf, sf, credit, ssem, rsem, lsem, tsem, trsem) = refs[24 + nb :]
    rep, fs, tp = lax.axis_index("rep"), lax.axis_index("fs"), lax.axis_index("tp")
    z, y, x = fs // 16, lax.rem(fs // 4, 4), lax.rem(fs, 4)
    pos = dict(x=x, y=y, z=z)
    mate = (rep, fs, 1 - tp)

    def beside(axis, sign):
        if axis == "x":
            return (rep, z * 16 + y * 4 + lax.rem(x + sign + 4, 4), tp)
        if axis == "y":
            return (rep, z * 16 + lax.rem(y + sign + 4, 4) * 4 + x, tp)
        far = lax.rem(rep * 2 + z + sign + 4, 4)
        return (far // 2, lax.rem(far, 2) * 16 + y * 4 + x, tp)

    local, at = [], 0
    for w in (wo, wi, wv, wp, wg, wu, wd):
        local.append(pltpu.make_async_copy(w, wf.at[:, pl.ds(at, w.shape[1])], lsem.at[len(local)]))
        at += w.shape[1]
    mine = pl.multiple_of(tp * 512, 512)
    other = pl.multiple_of((1 - tp) * 512, 512)
    local.append(pltpu.make_async_copy(tok.at[0], tt.at[pl.ds(mine, 512)], lsem.at[len(local)]))
    for c in local:
        c.start()

    barrier = pltpu.get_barrier_semaphore()
    for axis in "xyz":
        for sign in (1, -1):
            pl.semaphore_signal(barrier, inc=1, device_id=beside(axis, sign), device_id_type=MESH)
    pl.semaphore_signal(barrier, inc=1, device_id=mate, device_id_type=MESH)

    def cast(kind):
        for i in dict(m=(0, 1, 2), o=(3,), g=(4, 5), d=(6,), s=())[kind]:
            local[i].wait()
        if kind == "s":
            sf[...] = jnp.zeros((16, 128), F32)
            for k, v in enumerate((s_o, s_i, s_v)):
                sf[k : k + 1, 0:16] = v[...]
            for k, v in enumerate((s_g, s_u)):
                sf[11 + k : 12 + k, 0:44] = v[...]
            low = pltpu.roll(sf[0:8, :], lax.rem(fs * 16, 128), 1)
            high = pltpu.roll(sf[8:16, :], lax.rem(fs * 44, 128), 1)
            bufs[home[parts_of("s")[0]][0]][z, y, x] = low + high
            return
        column = None
        if kind in "od":
            eye = lax.broadcasted_iota(jnp.int32, (64, 64), 0) == lax.broadcasted_iota(jnp.int32, (64, 64), 1)
            column = jnp.sum(jnp.where(eye, (s_p if kind == "o" else s_d)[...], 0.0), axis=1, keepdims=True)
        j = 0
        for p in parts_of(kind):
            for b in range(PARTS[p][1]):
                if kind == "m":
                    v = wf[:, pl.ds((j % 3) * 512 + j // 3 * 128, 128)]
                elif kind == "g":
                    v = wf[:, pl.ds(2048 + (j % 2) * 1408 + j // 2 * 128, 128)]
                else:
                    v = wf[:, pl.ds((1536 if kind == "o" else 2048 + 2816) + j * 128, 128)] * column
                at = home[p][1] + b * 128
                bufs[home[p][0]][z, y, x, :, at : at + 128] = v.astype(BF)
                j += 1

    cast("s")
    cast("m")
    pl.semaphore_wait(barrier, 7)

    def to_mate(src, dst, k):
        return pltpu.make_async_remote_copy(
            src_ref=src, dst_ref=dst, send_sem=tsem.at[k], recv_sem=trsem.at[k], device_id=mate, device_id_type=MESH
        )

    tokens_over = to_mate(tok.at[0], tt.at[pl.ds(mine, 512)], 0)
    tokens_over.start()

    def where(spec, axis):
        v = spec[axis]
        if v == "all":
            return pl.ds(0, 2 if axis == "z" else 4)
        if v == "own":
            return pl.ds(pos[axis], 1)
        return pl.ds(lax.rem(pos[axis] + v + 4, 4), 1)

    def rows_of(i, size):
        return pl.ds(pl.multiple_of(i * size, size), size)

    def whole(p, cols):
        return bufs[home[p][0]][:, :, :, :, cols].reshape(2048, -1)

    def run_norm(h):
        if h == 0:
            local[-1].wait()
            tokens_over.wait()

        @pl.loop(h * 4, h * 4 + 4)
        def _(i):
            r = rows_of(i, 64)
            v = tt[r, :].astype(F32)
            v = v * lax.rsqrt(jnp.mean(v * v, axis=1, keepdims=True) + EPS) * mixg[...]
            xx[r, :] = v.astype(BF)

    def run_scales(p):
        lane = lax.broadcasted_iota(jnp.int32, (1, 128), 1)
        for k in range(3):
            for b in range(4):
                total = None
                for d in range(8 * b, 8 * b + 8):
                    v = bufs[home[p][0]][d // 16, d // 4 % 4, d % 4, k : k + 1, :]
                    total = v if total is None else total + v
                sc[k : k + 1, b * 128 : b * 128 + 128] = total
        for k in range(3, 5):
            for b in range(11):
                total = jnp.zeros((1, 128), F32)
                for d in range(32):
                    low, high = max(44 * d - 128 * b, 0), min(44 * d + 44 - 128 * b, 128)
                    if low < high:
                        v = bufs[home[p][0]][d // 16, d // 4 % 4, d % 4, k : k + 1, :]
                        total = jnp.where((lane >= low) & (lane < high), v, total)
                sc[k : k + 1, b * 128 : b * 128 + 128] = total

    def run_m(c, p):
        consts = []
        for h in range(2):
            cols = slice(c * 256 + h * 128, c * 256 + h * 128 + 128)
            consts.append((cols, mtaps[:, cols] * (sc[0:1, cols] * sc[1:2, cols] * sc[2:3, cols]), cgain[:, cols]))

        def tile(i, prev):
            r = rows_of(i, TM)
            acc = jnp.dot(xx[r, :], whole(p, slice(None)), preferred_element_type=F32)
            kept = []
            for h, (cols, taps, gain) in enumerate(consts):
                at = h * 384
                cur = acc[:, at + 128 : at + 256] * acc[:, at + 256 : at + 384]
                conv = acc[:, at : at + 128] * shifted_sum(prev[h], cur, taps)
                if c + h == 0:
                    ss[r, :] = conv * conv
                else:
                    ss[r, :] += conv * conv
                cc[r, cols] = (conv * gain).astype(BF)
                kept.append(cur[TM - 8 :])
            return tuple(kept)

        zero = jnp.zeros((8, 128), F32)
        lax.fori_loop(0, 1024 // TM, tile, (zero, zero))

    def p_over(q):
        c = pl.ds(q * 512, 512)
        return to_mate(ps.at[:, c], pr.at[:, c], 2 + q)

    squares_over = to_mate(ss, ssr, 1)

    def eighths(p, q):
        return bufs[home[p][0]][q // 2, pl.ds(q % 2 * 2, 2)].reshape(512, -1)

    def run_o(q):
        (p,) = parts_of("o")
        if q == 0:
            squares_over.start()
        ps[:, q * 512 : q * 512 + 512] = dot_nt(cc[...], eighths(p, q)).astype(BF)
        if q:
            p_over(q - 1).start()
        if q == 3:
            p_over(3).start()

    def run_f(i):
        if i == 0:
            squares_over.wait()
            for q in range(4):
                p_over(q).wait()

        @pl.loop(i * 4, i * 4 + 4)
        def _(k):
            r = rows_of(k, 64)
            row = lax.rsqrt(jnp.sum(ss[r, :] + ssr[r, :], axis=1, keepdims=True) * (1.0 / 1024) + EPS)
            v = tt[r, :].astype(F32) + row * (ps[r, :].astype(F32) + pr[r, :].astype(F32))
            b = v.astype(BF)
            tt[r, :] = b
            v = b.astype(F32)
            v = v * lax.rsqrt(jnp.mean(v * v, axis=1, keepdims=True) + EPS) * fgain[...]
            xx[r, :] = v.astype(BF)

        if i == 3:
            pl.semaphore_signal(credit, inc=1, device_id=mate, device_id_type=MESH)

    def run_g(j, p, b):
        cols = slice(j * 128, j * 128 + 128)
        tg, tu, bg, bu = gtaps[:, cols], utaps[:, cols], gbias[cols][None], ubias[cols][None]
        sg, su = sc[3:4, cols], sc[4:5, cols]

        tg, tu = tg * sg, tu * su

        def tile(i, prev):
            r = rows_of(i, TM)
            acc = jnp.dot(xx[r, :], whole(p, slice(b * 256, b * 256 + 256)), preferred_element_type=F32)
            g, u = acc[:, :128], acc[:, 128:]
            ga = shifted_sum(prev[0], g, tg) + bg
            ua = shifted_sum(prev[1], u, tu) + bu
            hh[r, cols] = (ga / (1.0 + jnp.exp(-ga)) * ua).astype(BF)
            return g[TM - 8 :], u[TM - 8 :]

        zero = jnp.zeros((8, 128), F32)
        lax.fori_loop(0, 1024 // TM, tile, (zero, zero))

    def run_d(p, k, first, q):
        w = eighths(p, q)
        v = dot_nt(hh[:, k : k + w.shape[1]], w)
        c = slice(q * 512, q * 512 + 512)
        yy[:, c] = v if first else yy[:, c] + v

    def d_over(q):
        c = pl.ds(q * 512, 512)
        return to_mate(ps.at[pl.ds(0, 512), c], pr.at[pl.ds(0, 512), c], 6 + q)

    def run_e(p, k):
        own, far = pl.ds(mine, 512), pl.ds(other, 512)
        for q in range(4):
            w = eighths(p, q)
            c = slice(q * 512, q * 512 + 512)
            ps[0:512, c] = (yy[far, c] + dot_nt(hh[far, k : k + w.shape[1]], w)).astype(BF)
            if q == 1:
                pl.semaphore_wait(credit, 1)
            if q:
                d_over(q - 1).start()
        d_over(3).start()
        for q in range(4):
            w = eighths(p, q)
            c = slice(q * 512, q * 512 + 512)
            yy[own, c] += dot_nt(hh[own, k : k + w.shape[1]], w)
            d_over(q).wait()

            @pl.loop(0, 8)
            def _(i):
                r = pl.ds(pl.multiple_of(mine + i * 64, 64), 64)
                o = rows_of(i, 64)
                out[0, o, c] = (tt[r, c].astype(F32) + yy[r, c] + pr[o, c].astype(F32)).astype(BF)

    steps, ends = plan(segments_of())
    started, got = {}, set()

    def arrived(keys):
        for key in keys:
            if key not in got and key[0] != "cast":
                got.add(key)
                started[key].wait_recv()

    scaled = False
    for what, it, _ in steps:
        if what == "send":
            arrived(it.deps)
            kind, blocks, _ = PARTS[it.part]
            b, at = home[it.part]
            ref = bufs[b].at[where(it.spec, "z"), where(it.spec, "y"), where(it.spec, "x"), pl.ds(*it.rows), pl.ds(at, max(blocks, 1) * 128)]
            c = pltpu.make_async_remote_copy(
                src_ref=ref,
                dst_ref=ref,
                send_sem=ssem.at[it.key],
                recv_sem=rsem.at[it.key],
                device_id=beside(it.axis, it.sign),
                device_id_type=MESH,
            )
            c.start()
            started[it.key] = c
            continue
        name, _, needs = it
        for p in needs:
            arrived(ends[p])
        if name[0] == "m" and not scaled:
            scaled = True
            run_scales(parts_of("s")[0])
        dict(cast=cast, norm=run_norm, m=run_m, o=run_o, f=run_f, g=run_g, d=run_d, e=run_e)[name[0]](*name[1:])
    for c in started.values():
        c.wait_send()


def local(
    tokens, mix_gain, out_gate_w, in_gate_w, value_w, out_gate_scale, in_gate_scale, value_scale, mix_taps, conv_gain,
    out_proj_w, proj_scale, ffn_gain, gate_w, up_w, gate_scale, up_scale, gate_taps, up_taps, gate_bias, up_bias, down_w, down_scale,
):
    n = len(PARTS)
    hbm, vmem = pl.BlockSpec(memory_space=pl.ANY), pl.BlockSpec(memory_space=pltpu.VMEM)
    bufs = [pltpu.VMEM((2, 4, 4, 64, w), BF) if w else pltpu.VMEM((2, 4, 4, 8, 128), F32) for w in homes()[1]]
    dma = pltpu.SemaphoreType.DMA
    return pl.pallas_call(
        kernel,
        out_shape=pltpu.VMEM((1, 512, 2048), BF),
        in_specs=[hbm] * 8 + [vmem] * 15,
        out_specs=vmem,
        scratch_shapes=bufs
        + [
            pltpu.VMEM((1024, 2048), BF),
            pltpu.VMEM((1024, 2048), BF),
            pltpu.VMEM((1024, 512), BF),
            pltpu.VMEM((1024, 128), F32),
            pltpu.VMEM((1024, 128), F32),
            pltpu.VMEM((1024, 2048), BF),
            pltpu.VMEM((1024, 2048), BF),
            pltpu.VMEM((1024, 1408), BF),
            pltpu.VMEM((1024, 2048), F32),
            pltpu.VMEM((8, 1408), F32),
            pltpu.VMEM((64, 6272), F32),
            pltpu.VMEM((16, 128), F32),
            pltpu.SemaphoreType.REGULAR,
            dma((n, 5, 2)),
            dma((n, 5, 2)),
            dma((8,)),
            dma((10,)),
            dma((10,)),
        ],
        compiler_params=pltpu.CompilerParams(collective_id=0, has_side_effects=True, vmem_limit_bytes=64600000),
        name="layer",
    )(
        tokens, out_gate_w, in_gate_w, value_w, out_proj_w.T, gate_w, up_w, down_w.T,
        out_gate_scale[None], in_gate_scale[None], value_scale[None], gate_scale[None], up_scale[None],
        proj_scale[None], down_scale[None], mix_gain[None], mix_taps, conv_gain[None], ffn_gain[None],
        gate_taps, up_taps, gate_bias, up_bias,
    )


def solution(mesh):
    placed = (
        P(("rep", "fs"), "tp", None),
        P(),
        P("fs", "tp"),
        P("fs", "tp"),
        P("fs", "tp"),
        P(("tp", "fs")),
        P(("tp", "fs")),
        P(("tp", "fs")),
        P(None, "tp"),
        P("tp"),
        P("tp", "fs"),
        P("fs"),
        P(),
        P("fs", "tp"),
        P("fs", "tp"),
        P(("tp", "fs")),
        P(("tp", "fs")),
        P(None, "tp"),
        P(None, "tp"),
        P("tp"),
        P("tp"),
        P("tp", "fs"),
        P("fs"),
    )
    return jax.shard_map(
        local, mesh=mesh, in_specs=placed, out_specs=P(("rep", "fs"), "tp", None), check_vma=False
    )
```
